128 devices in a mesh: sp: 16 (over z, x), tp: 8 (over y, core).
Axes of the slice: x: 4, y: 4, z: 4, core: 2. Of those that a mesh axis runs over, the one named last changes fastest.
Arguments:
- target: bfloat16 [8192, 4096], P(('sp', 'tp')), may hold values from -0.07 to 0.07
- source: bfloat16 [16384, 4096], P(('sp', 'tp')), may hold values from -0.035 to 0.035
- gain_target: float32 [4096], replicated, may hold values from 0.1 to 1.9
- gain_source: float32 [4096], replicated, may hold values from 0.1 to 1.9
- w_query: bfloat16 [4096, 1024], P(None, 'tp'), may hold values from -1 to 1
- w_key: bfloat16 [4096, 512], replicated, may hold values from -1 to 1
- w_value: bfloat16 [4096, 512], replicated, may hold values from -0.09375 to 0.09375
- w_out: bfloat16 [1024, 4096], P('tp'), may hold values from -0.1875 to 0.1875
- grad_output: bfloat16 [8192, 4096], P(('sp', 'tp')), may hold values from -6 to 6
Outputs:
- grad_target: float32 [8192, 4096], P(('sp', 'tp'))
- grad_source: float32 [16384, 4096], P(('sp', 'tp'))
- grad_out_proj: float32 [1024, 4096], P('tp')
The draws below stay inside these ranges and needn't reach their ends.
All inputs are finite; a program needn't handle non-finite values.
Results may differ from the reference program's by a relative error of at most 0.028.
Values may be sent and summed in bfloat16 or wider, within the bound.
A program may use at most 128 MiB of HBM per device.

```python
import jax
import jax.numpy as jnp
from jax import lax

D = 4096
HQ = 16
HK = 8
HD = 64
TGT_ROWS = 8192
SRC_ROWS = 16384


def aligned_draw(key):
    query_weight = jnp.clip(jax.random.normal(jax.random.fold_in(key, 11), (D, HQ * HD), jnp.float32), -6.0, 6.0) * float(D) ** (-0.5)
    key_weight = jnp.clip(jax.random.normal(jax.random.fold_in(key, 12), (D, HK * HD), jnp.float32), -6.0, 6.0) * float(D) ** (-0.5)
    target_rows = jnp.clip(jax.random.normal(jax.random.fold_in(key, 13), (TGT_ROWS, D), jnp.float32), -6.0, 6.0) * 0.01
    source_rows = jnp.clip(jax.random.normal(jax.random.fold_in(key, 14), (SRC_ROWS, D), jnp.float32), -6.0, 6.0) * 0.005
    return (query_weight, key_weight, jnp.clip(target_rows, -0.07, 0.07), jnp.clip(source_rows, -0.035, 0.035))


def draw_target(key, part):
    return aligned_draw(key)[2].astype(jnp.bfloat16)


def draw_source(key, part):
    return aligned_draw(key)[3].astype(jnp.bfloat16)


def draw_w_query(key, part):
    return aligned_draw(key)[0].astype(jnp.bfloat16)


def draw_w_key(key, part):
    return aligned_draw(key)[1].astype(jnp.bfloat16)


def block_levels(stream_key, extent, split, least, largest):
    factor_of, own = 1.0, jax.random.fold_in(stream_key, 6)
    for dim, shards_of in split:
        draws = jnp.exp(jax.random.uniform(jax.random.fold_in(own, dim), (shards_of,), jnp.float32, least / len(split), largest / len(split)))
        factor_of = factor_of * jnp.repeat(draws, extent[dim] // shards_of).reshape([-1 if axis == dim else 1 for axis in range(len(extent))])
    return factor_of


def scatter_about(rng, extent, spread, most, split=(), held_as=jnp.bfloat16):
    factor_of = block_levels(rng, extent, split, -0.22, 0.18) if split else 1.0
    array = jax.random.normal(rng, extent, jnp.float32) * spread * factor_of
    return jnp.minimum(jnp.maximum(array, -most), most).astype(held_as)


def setup_inputs(seed: int = 0) -> dict:
    streams_of = jax.random.split(jax.random.key(seed), 10)
    target = draw_target(jax.random.fold_in(streams_of[9], 71), 0)
    source = draw_source(jax.random.fold_in(streams_of[9], 71), 0)
    gain_target = jnp.clip(1.0 + 0.18 * jax.random.normal(streams_of[2], (D,), jnp.float32), 0.1, 1.9)
    gain_source = jnp.clip(1.0 + 0.18 * jax.random.normal(streams_of[3], (D,), jnp.float32), 0.1, 1.9)
    w_query = draw_w_query(jax.random.fold_in(streams_of[9], 71), 0)
    w_key = draw_w_key(jax.random.fold_in(streams_of[9], 71), 0)
    w_value = scatter_about(streams_of[6], (D, HK * HD), D ** -0.5, 0.09375)
    w_out = scatter_about(streams_of[7], (HQ * HD, D), (HQ * HD) ** -0.5, 0.1875, ((0, 8),))
    grad_output = scatter_about(streams_of[8], (TGT_ROWS, D), 1.0, 6.0, ((0, 128),))
    return dict(target=target, source=source, gain_target=gain_target, gain_source=gain_source, w_query=w_query, w_key=w_key, w_value=w_value, w_out=w_out, grad_output=grad_output)


EPS = 1e-06

def normalize(matrix, scaling):
    widened = matrix.astype(jnp.float32)
    factor = lax.rsqrt(lax.optimization_barrier(jnp.mean(widened * widened, axis=-1, keepdims=True)) + EPS)
    return (widened * factor * scaling.astype(jnp.float32)).astype(jnp.bfloat16)

def norm_back(matrix, scaling, upstream):
    widened = matrix.astype(jnp.float32)
    factor = lax.rsqrt(lax.optimization_barrier(jnp.mean(widened * widened, axis=-1, keepdims=True)) + EPS)
    weighted = upstream * scaling.astype(jnp.float32)
    inner = lax.optimization_barrier(jnp.mean(widened * weighted, axis=-1, keepdims=True))
    return factor * weighted - widened * factor * factor * factor * inner

def reference(target, source, gain_target, gain_source, w_query, w_key, w_value, w_out, grad_output):
    contract_last = (((1,), (1,)), ((), ()))
    normed_target = normalize(target, gain_target)
    normed_source = normalize(source, gain_source)
    query = jnp.dot(normed_target, w_query, preferred_element_type=jnp.float32).astype(jnp.bfloat16)
    keys_all = jnp.dot(normed_source, w_key, preferred_element_type=jnp.float32).astype(jnp.bfloat16)
    values_all = jnp.dot(normed_source, w_value, preferred_element_type=jnp.float32).astype(jnp.bfloat16)
    head_grads = lax.dot_general(grad_output, w_out, contract_last, preferred_element_type=jnp.float32).astype(jnp.bfloat16)
    target_count = target.shape[0]
    source_count = source.shape[0]
    group_size = HQ // HK
    score_scale = float(HD) ** (-0.5)
    query_heads = query.reshape(target_count, HQ, HD).transpose(1, 0, 2)
    grad_heads = head_grads.reshape(target_count, HQ, HD).transpose(1, 0, 2)
    key_heads = keys_all.reshape(source_count, HK, HD).transpose(1, 0, 2)
    value_heads = values_all.reshape(source_count, HK, HD).transpose(1, 0, 2)

    def one_head(bundle):
        query_head, grad_head, position = bundle
        key_head = key_heads[position]
        value_head = value_heads[position]
        scores = jnp.dot(query_head, key_head.T, preferred_element_type=jnp.float32) * score_scale
        maxima = lax.optimization_barrier(jnp.max(scores, axis=-1, keepdims=True))
        weights = jnp.exp(scores - maxima)
        totals = lax.optimization_barrier(jnp.sum(weights, axis=-1, keepdims=True))
        output = (jnp.dot(weights.astype(jnp.bfloat16), value_head, preferred_element_type=jnp.float32) / totals).astype(jnp.bfloat16)
        attend = weights / totals
        delta_sum = lax.optimization_barrier(jnp.sum(grad_head.astype(jnp.float32) * output.astype(jnp.float32), axis=-1, keepdims=True))
        grad_attend = jnp.dot(grad_head, value_head.T, preferred_element_type=jnp.float32)
        mixed = (attend * (grad_attend - delta_sum) * score_scale).astype(jnp.bfloat16)
        grad_query = jnp.dot(mixed, key_head, preferred_element_type=jnp.float32).astype(jnp.bfloat16)
        grad_key = jnp.dot(mixed.T, query_head, preferred_element_type=jnp.float32)
        grad_value = jnp.dot(attend.astype(jnp.bfloat16).T, grad_head, preferred_element_type=jnp.float32)
        return (output, grad_query, grad_key, grad_value)
    positions = jnp.arange(HQ, dtype=jnp.int32) // group_size
    output, grad_query, grad_key, grad_value = lax.map(one_head, (query_heads, grad_heads, positions))
    attention = output.transpose(1, 0, 2).reshape(target_count, HQ * HD)
    query_grads = grad_query.transpose(1, 0, 2).reshape(target_count, HQ * HD)
    key_grads = lax.optimization_barrier(jnp.sum(grad_key.reshape(HK, group_size, source_count, HD), axis=1)).astype(jnp.bfloat16)
    key_grads = key_grads.transpose(1, 0, 2).reshape(source_count, HK * HD)
    value_grads = lax.optimization_barrier(jnp.sum(grad_value.reshape(HK, group_size, source_count, HD), axis=1)).astype(jnp.bfloat16)
    value_grads = value_grads.transpose(1, 0, 2).reshape(source_count, HK * HD)
    grad_xn = lax.dot_general(query_grads, w_query, contract_last, preferred_element_type=jnp.float32)
    grad_target = norm_back(target, gain_target, grad_xn)
    grad_sn = lax.dot_general(key_grads, w_key, contract_last, preferred_element_type=jnp.float32)
    grad_sn = grad_sn + lax.dot_general(value_grads, w_value, contract_last, preferred_element_type=jnp.float32)
    grad_source = norm_back(source, gain_source, grad_sn)
    grad_out_proj = lax.dot_general(attention, grad_output, (((0,), (0,)), ((), ())), preferred_element_type=jnp.float32)
    return (grad_target, grad_source, grad_out_proj)
```

```python
import functools

import jax
import jax.numpy as jnp
from jax import lax
from jax.experimental import pallas as pl
from jax.experimental.pallas import tpu as pltpu
from jax.sharding import PartitionSpec as P

BF = jnp.bfloat16
F32 = jnp.float32
EPS = 1e-06
MESH = pl.DeviceIdType.MESH

T = 512
TT = 2 * T
U = 1024
XN0 = 4096


def dot(a, b):
    return jnp.dot(a, b, preferred_element_type=F32)


def dot_t(a, b):
    return lax.dot_general(a, b, (((1,), (1,)), ((), ())), preferred_element_type=F32)


def normalize(rows, gain):
    wide = rows.astype(F32)
    factor = lax.rsqrt(jnp.mean(wide * wide, axis=-1, keepdims=True) + EPS)
    return (wide * factor * gain).astype(BF)


def order(i):
    return i + i // 2 - 2 * (i // 3)


class Coords:
    def __init__(self):
        self.sp = lax.axis_index("sp")
        self.tp = lax.axis_index("tp")
        self.z, self.x = self.sp // 4, self.sp % 4
        self.y, self.c = self.tp // 2, self.tp % 2

    def block(self, half, a, b):
        if half == 0:
            return ((self.z + b) % 4) * 4 + (self.x + a) % 4
        return ((self.z + a) % 4) * 4 + (self.x + b) % 4

    def ring(self, d, sib):
        return ((self.y + d) % 4) * 2 + (self.c if sib == 0 else 1 - self.c)


class Net:
    def __init__(self, at, send_sems, stand_in):
        self.at, self.sems, self.count, self.stand_in = at, send_sems, 0, stand_in

    def push(self, src, dst, recv, sp=None, tp=None):
        number = self.count
        sem = self.sems.at[number]
        self.count += 1
        who = (self.at.sp if sp is None else sp, self.at.tp if tp is None else tp)
        copy = pltpu.make_async_remote_copy(
            src_ref=src, dst_ref=dst, send_sem=sem, recv_sem=recv, device_id=who, device_id_type=MESH
        )
        copy.start()
        return number, src.shape

    def sent(self, copies):
        for number, (rows, columns) in copies:
            place = self.stand_in.at[pl.ds(0, rows), pl.ds(0, columns)]
            pltpu.make_async_remote_copy(
                src_ref=place, dst_ref=place, send_sem=self.sems.at[number], recv_sem=self.sems.at[number],
                device_id=(self.at.sp, self.at.ring(1, 0)), device_id_type=MESH,
            ).wait_send()

    def arrive(self, dst, recv):
        pltpu.make_async_remote_copy(
            src_ref=dst, dst_ref=dst, send_sem=self.sems.at[0], recv_sem=recv,
            device_id=(self.at.sp, self.at.ring(1, 0)), device_id_type=MESH,
        ).wait_recv()


class RowsGather:
    def __init__(self, net, place, recv):
        self.net, self.place, self.recv = net, place, recv

    def send(self, d, h, way):
        at = self.net.at
        src = self.place(at.ring(d, 0), h)
        if way == 0:
            return self.net.push(src, src, self.recv.at[d, 1, h], tp=at.ring(0, 1))
        return self.net.push(src, src, self.recv.at[(d - way) % 4, 0, h], tp=at.ring(way, 0))

    def begin(self):
        s = self.send
        return [s(0, 0, 1), s(0, 1, -1), s(0, 1, 1), s(0, 0, -1), s(0, 0, 0), s(0, 1, 0)]

    def come(self, d, h, sib):
        at = self.net.at
        self.net.arrive(self.place(at.ring(d, sib), h), self.recv.at[d, sib, h])
        sent = []
        if sib == 0:
            if (d, h) == (3, 0):
                sent.append(self.send(d, h, 1))
            if (d, h) == (1, 1):
                sent.append(self.send(d, h, -1))
            sent.append(self.send(d, h, 0))
        return sent


FIRST = [(3, 0), (1, 1)]
SECOND = [(3, 1), (1, 0), (2, 0), (2, 1)]
SIBS = [(0, 0), (0, 1), (3, 0), (1, 1), (3, 1), (1, 0), (2, 0), (2, 1)]


class PairsGather:
    def __init__(self, net, kv, recv):
        self.net, self.kv, self.recv = net, kv, recv

    def rows(self, half, a, b, piece):
        start = self.net.at.block(half, a, b) * 1024 + half * 512 + piece * 256
        return self.kv.at[pl.ds(pl.multiple_of(start, 256), 256), :]

    def send(self, half, a, b, piece, axis, way):
        at = self.net.at
        src = self.rows(half, a, b, piece)
        if axis == 0:
            to, a2, b2 = at.block(half, way, 0), (a - way) % 4, b
        else:
            to, a2, b2 = at.block(half, 0, way), a, (b - way) % 4
        return self.net.push(src, src, self.recv.at[half, a2, b2, piece], sp=to)

    def begin(self):
        sent = []
        for piece, way in ((0, 1), (1, -1), (1, 1), (0, -1)):
            for half in (0, 1):
                sent.append(self.send(half, 0, 0, piece, 0, way))
        for piece, way in ((0, 1), (1, -1), (1, 1), (0, -1)):
            for half in (0, 1):
                sent.append(self.send(half, 0, 0, piece, 1, way))
        return sent

    def come(self, a, b, piece):
        sent = []
        for half in (0, 1):
            self.net.arrive(self.rows(half, a, b, piece), self.recv.at[half, a, b, piece])
            if b == 0:
                if (a, piece) == (3, 0):
                    sent.append(self.send(half, a, b, piece, 0, 1))
                if (a, piece) == (1, 1):
                    sent.append(self.send(half, a, b, piece, 0, -1))
                for way in (1, -1):
                    sent.append(self.send(half, a, b, piece, 1, way))
            else:
                if (b, piece) == (3, 0):
                    sent.append(self.send(half, a, b, piece, 1, 1))
                if (b, piece) == (1, 1):
                    sent.append(self.send(half, a, b, piece, 1, -1))
        return sent


PHASE1 = [(3, 0, 0), (1, 0, 1), (3, 0, 1), (1, 0, 0), (2, 0, 0), (2, 0, 1)]
PHASE2 = (
    [(0, 3, 0), (0, 1, 1), (0, 3, 1), (0, 1, 0)]
    + [e for a in (3, 1) for e in ((a, 3, 0), (a, 1, 1), (a, 3, 1), (a, 1, 0))]
    + [(0, 2, 0), (0, 2, 1)]
    + [(2, 3, 0), (2, 1, 1), (2, 3, 1), (2, 1, 0)]
    + [e for a in (3, 1, 2) for e in ((a, 2, 0), (a, 2, 1))]
)


def kernel(
    tgt, src, gain_t, gain_s, wq, wk, wv, wo, go,
    wq_all, gop, dq_loc, dkv_loc,
    E, kv, gg, dkv, hop, end1, hop2, end2, ar1, ar2,
    qT, qP, dT, dP, acc, m_run, m_unit, dqT, oT, pr, back, fin, dqs,
    tgt_v, wo_v, gt_v, gs_v,
    send_sems, load_sems, r_xn, r_gg, r_wq, r_a2a, r_kv, r_rs1, r_rs2, r_rs3, r_rs4, r_ar, r_dq, r_dkv,
):
    src_v = gop
    arP = wo_v
    at = Coords()
    net = Net(at, send_sems, E)
    lane = lax.broadcasted_iota(jnp.int32, (1, 128), 1)
    low = lane < 64

    barrier = pltpu.get_barrier_semaphore()
    others = [(at.sp, (at.tp + j) % 8) for j in range(1, 8)]
    others += [(at.block(0, a, 0), at.tp) for a in (1, 2, 3)]
    others += [(at.block(0, 0, b), at.tp) for b in (1, 2, 3)]
    for who in others:
        pl.semaphore_signal(barrier, inc=1, device_id=who, device_id_type=MESH)

    gg_own = [
        pltpu.make_async_copy(
            go.at[:, pl.ds(1024 * k, 1024)],
            gg.at[pl.ds(pl.multiple_of(at.tp * 256 + 64 * k, 64), 64), :],
            load_sems.at[8 + k],
        )
        for k in range(4)
    ]
    loads = [
        pltpu.make_async_copy(tgt, tgt_v, load_sems.at[0]),
        pltpu.make_async_copy(gain_t, gt_v, load_sems.at[1]),
        pltpu.make_async_copy(src, src_v, load_sems.at[2]),
        pltpu.make_async_copy(gain_s, gs_v, load_sems.at[3]),
        pltpu.make_async_copy(wk, E.at[pl.ds(0, 4096), pl.ds(0, 512)], load_sems.at[4]),
        pltpu.make_async_copy(wv, E.at[pl.ds(0, 4096), pl.ds(512, 512)], load_sems.at[5]),
        pltpu.make_async_copy(wo, wo_v, load_sems.at[6]),
    ]
    loads_w = [
        pltpu.make_async_copy(
            wq.at[pl.ds(512 * k, 512), :], dkv.at[0, k // 4, k % 4], load_sems.at[16 + k]
        )
        for k in range(8)
    ]
    for load in loads + loads_w + gg_own:
        load.start()

    def xn_place(j, h):
        return E.at[pl.ds(pl.multiple_of(XN0 + j * 256 + h * 128, 128), 128), :]

    def gg_place(j, h):
        return gg.at[pl.ds(pl.multiple_of(j * 256 + h * 128, 128), 128), :]

    def wq_place(j, h):
        return wq_all.at[j, pl.ds(h * 2048, 2048), :]

    rows_x = RowsGather(net, xn_place, r_xn)
    rows_g = RowsGather(net, gg_place, r_gg)
    rows_w = RowsGather(net, wq_place, r_wq)

    loads[0].wait()
    loads[1].wait()
    xn = normalize(tgt_v[...], gt_v[...])
    for k in range(4):
        E[pl.ds(pl.multiple_of(XN0 + at.tp * 256 + 64 * k, 64), 64), :] = xn[:, 1024 * k : 1024 * k + 1024]
    pl.semaphore_wait(barrier, len(others))
    sent_x = rows_x.begin()

    loads[2].wait()
    loads[3].wait()
    sn = normalize(src_v[...], gs_v[...])
    loads[4].wait()
    loads[5].wait()
    pairs = dot(sn, E[0:4096, :])
    for g in range(4):
        kb = pairs[:, 128 * g : 128 * g + 128]
        vb = pairs[:, 512 + 128 * g : 512 + 128 * g + 128]
        pr[2 * g] = jnp.where(low, kb, pltpu.roll(vb, 64, 1)).astype(BF)
        pr[2 * g + 1] = jnp.where(low, pltpu.roll(kb, 64, 1), vb).astype(BF)
    mine = kv.at[pl.ds(pl.multiple_of(at.sp * 1024 + at.tp * 128, 128), 128), :]
    sent = []
    for j in (4, 3, 5, 2, 6, 1, 7):
        to = (at.tp + j) % 8
        sent.append(net.push(pr.at[to], mine, r_a2a.at[8 - j], tp=to))
    mine[...] = pr[at.tp]
    for j in range(1, 8):
        frm = (at.tp + j) % 8
        net.arrive(kv.at[pl.ds(pl.multiple_of(at.sp * 1024 + frm * 128, 128), 128), :], r_a2a.at[j])
    pairs_g = PairsGather(net, kv, r_kv)
    sent += pairs_g.begin()
    for load in gg_own:
        load.wait()
    loads[6].wait()
    for load in loads_w:
        load.wait()
    own_w = [
        pltpu.make_async_copy(
            dkv.at[0, k // 4, k % 4], wq_all.at[at.tp, pl.ds(512 * k, 512), :], load_sems.at[24 + k]
        )
        for k in range(8)
    ]
    for copy in own_w:
        copy.start()

    for d, h in FIRST:
        sent_x += rows_x.come(d, h, 0)
    sent += rows_g.begin()
    for e in PHASE1:
        sent += pairs_g.come(*e)
    for d, h in SECOND:
        sent_x += rows_x.come(d, h, 0)
    for e in PHASE2:
        sent += pairs_g.come(*e)
    for d, h in SIBS:
        rows_x.come(d, h, 1)

    def gathered(ref, base, k):
        return jnp.concatenate(
            [ref[base + j * 256 + k * 64 : base + j * 256 + k * 64 + 64, :] for j in range(8)], axis=0
        )

    def wq_rows(k):
        return jnp.concatenate([dkv[0, k // 2, 2 * (k % 2)], dkv[0, k // 2, 2 * (k % 2) + 1]], axis=0)

    q = dot(gathered(E, XN0, 0), wq_rows(0))
    for k in range(1, 4):
        q += dot(gathered(E, XN0, k), wq_rows(k))
    q = q.astype(BF).astype(F32)
    net.sent(sent_x)

    for d, h in FIRST:
        sent += rows_g.come(d, h, 0)
    for copy in own_w:
        copy.wait()
    sent += rows_w.begin()
    for d, h in SECOND:
        sent += rows_g.come(d, h, 0)
    for d, h in SIBS:
        rows_g.come(d, h, 1)
    do = dot_t(gathered(gg, 0, 0), wo_v[:, 0:1024])
    for k in range(1, 4):
        do += dot_t(gathered(gg, 0, k), wo_v[:, 1024 * k : 1024 * k + 1024])
    do = do.astype(BF).astype(F32)

    q0 = jnp.where(low, q, 0.0)
    q1 = jnp.where(low, pltpu.roll(q, 64, 1), 0.0)
    d0 = jnp.where(low, 0.0, pltpu.roll(do, 64, 1))
    d1 = jnp.where(low, 0.0, do)
    for h, (a, b) in enumerate(((q0, d0), (q1, d1))):
        r = slice(h * T, h * T + T)
        qP[r, :] = a.astype(BF)
        dP[r, :] = b.astype(BF)
        qT[:, r] = (a * 0.125).T.astype(BF)
        dT[:, r] = (b * 0.125).T.astype(BF)

    acc[...] = jnp.zeros_like(acc)
    m_run[...] = jnp.full_like(m_run, -jnp.inf)
    dqT[...] = jnp.zeros_like(dqT)
    ones = jnp.ones((16, U), BF)

    def unit_kv(a, b):
        parts = []
        for half in (0, 1):
            start = pl.multiple_of(at.block(half, a, b) * 1024 + half * 512, 512)
            parts.append(kv[pl.ds(start, 512), :])
        return jnp.concatenate(parts, axis=0)

    def fwd(u, _):
        block = unit_kv(order(u % 4), order(u // 4))
        s = dot(block, qT[...])
        m_old = m_run[...]
        m_new = jnp.maximum(m_old, jnp.max(s, axis=0, keepdims=True))
        shrink = jnp.exp(m_old - m_new)
        e = jnp.exp(s - m_new).astype(BF)
        E[pl.ds(pl.multiple_of(u * U, U), U), :] = e
        m_run[...] = m_new
        m_unit[pl.ds(u, 1)] = m_new[None]
        vt = block.astype(F32).T.astype(BF)[64:128, :]
        acc[...] = acc[...] * shrink + dot(jnp.concatenate([vt, ones], axis=0), e)
        return 0

    lax.fori_loop(0, 16, fwd, 0)
    inv = 1.0 / acc[64:65, :]
    o = (acc[0:64, :] * inv).astype(BF)
    oT[0:64, :] = o[:, 0:T]
    oT[64:128, :] = o[:, T:]
    delta = jnp.sum(dT[64:128, :].astype(F32) * o.astype(F32), axis=0, keepdims=True)
    m_end = m_run[...]

    for k in range(4):
        arP[:, 1024 * k : 1024 * k + 1024] = dot(oT[...], gathered(gg, 0, k)).astype(BF)

    def wide_col(half, a):
        pi = at.x if half == 0 else at.z
        return pl.ds(pl.multiple_of(half * 2048 + ((pi + a) % 4) * 512, 512), 512)

    def slim_col(half, b):
        pi, qi = (at.x, at.z) if half == 0 else (at.z, at.x)
        return pl.ds(pl.multiple_of(half * 2048 + pi * 512 + ((qi + b) % 4) * 128, 128), 128)

    def ar_1():
        for half in (0, 1):
            for a in (1, 3, 2):
                sent.append(net.push(arP.at[:, wide_col(half, a)], ar1.at[half, 4 - a], r_ar.at[0, half, 4 - a], sp=at.block(half, a, 0)))

    def ar_2():
        for half in (0, 1):
            total = arP[:, wide_col(half, 0)].astype(F32)
            for a in (1, 2, 3):
                net.arrive(ar1.at[half, a], r_ar.at[0, half, a])
                total += ar1[half, a].astype(F32)
            arP[:, wide_col(half, 0)] = total.astype(BF)
            for b in (1, 3, 2):
                sent.append(net.push(arP.at[:, slim_col(half, b)], ar2.at[half, 4 - b], r_ar.at[1, half, 4 - b], sp=at.block(half, 0, b)))

    def ar_3():
        for half in (0, 1):
            total = arP[:, slim_col(half, 0)].astype(F32)
            for b in (1, 2, 3):
                net.arrive(ar2.at[half, b], r_ar.at[1, half, b])
                total += ar2[half, b].astype(F32)
            gop[:, slim_col(half, 0)] = total.astype(BF)
            for b in (1, 3, 2):
                place = gop.at[:, slim_col(half, 0)]
                sent.append(net.push(place, place, r_ar.at[2, half, 4 - b], sp=at.block(half, 0, b)))

    def ar_4():
        for half in (0, 1):
            for b in (1, 2, 3):
                net.arrive(gop.at[:, slim_col(half, b)], r_ar.at[2, half, b])
            for a in (1, 3, 2):
                place = gop.at[:, wide_col(half, 0)]
                sent.append(net.push(place, place, r_ar.at[3, half, 4 - a], sp=at.block(half, a, 0)))

    def ar_5():
        for half in (0, 1):
            for a in (1, 2, 3):
                net.arrive(gop.at[:, wide_col(half, a)], r_ar.at[3, half, a])

    def add_to(place, arrived):
        place[...] = (place[...].astype(F32) + arrived[...].astype(F32)).astype(BF)

    def after(i):
        a, b = [2, 3, 1, 0][i // 4], [2, 3, 1, 0][i % 4]
        for half in (0, 1):
            piece = dkv.at[half, a, b]
            top, bottom = piece.at[pl.ds(0, 256), :], piece.at[pl.ds(256, 256), :]
            plus, minus = at.block(half, 1, 0), at.block(half, 3, 0)
            plus2, minus2 = at.block(half, 0, 1), at.block(half, 0, 3)
            if a == 2:
                sent.append(net.push(top, hop.at[half, 0, b], r_rs1.at[half, 0, b], sp=plus))
                sent.append(net.push(bottom, hop.at[half, 1, b], r_rs1.at[half, 1, b], sp=minus))
            elif a == 3:
                net.arrive(hop.at[half, 1, b], r_rs1.at[half, 1, b])
                add_to(bottom, hop.at[half, 1, b])
                sent.append(net.push(piece, end1.at[half, 1, b], r_rs2.at[half, 1, b], sp=minus))
            elif a == 1:
                net.arrive(hop.at[half, 0, b], r_rs1.at[half, 0, b])
                add_to(top, hop.at[half, 0, b])
                sent.append(net.push(piece, end1.at[half, 0, b], r_rs2.at[half, 0, b], sp=plus))
            else:
                total = piece[...].astype(F32)
                for side in (0, 1):
                    net.arrive(end1.at[half, side, b], r_rs2.at[half, side, b])
                    total += end1[half, side, b].astype(F32)
                if b == 2:
                    piece[...] = total.astype(BF)
                    sent.append(net.push(top, hop2.at[half, 0], r_rs3.at[half, 0], sp=plus2))
                    sent.append(net.push(bottom, hop2.at[half, 1], r_rs3.at[half, 1], sp=minus2))
                elif b == 3:
                    piece[...] = total.astype(BF)
                    net.arrive(hop2.at[half, 1], r_rs3.at[half, 1])
                    add_to(bottom, hop2.at[half, 1])
                    sent.append(net.push(piece, end2.at[half, 1], r_rs4.at[half, 1], sp=minus2))
                elif b == 1:
                    piece[...] = total.astype(BF)
                    net.arrive(hop2.at[half, 0], r_rs3.at[half, 0])
                    add_to(top, hop2.at[half, 0])
                    sent.append(net.push(piece, end2.at[half, 0], r_rs4.at[half, 0], sp=plus2))
                else:
                    for side in (0, 1):
                        net.arrive(end2.at[half, side], r_rs4.at[half, side])
                        total += end2[half, side].astype(F32)
                    fin[half * 512 : half * 512 + 512, :] = total.astype(BF)

    def bwd(i, _):
        for k in range(16):
            if k == 3:
                extra = [ar_2]
            elif k == 6:
                extra = [ar_3]
            elif k == 8:
                extra = [ar_4]
            else:
                extra = []

            @pl.when(i == k)
            def _(k=k, extra=extra):
                for f in extra:
                    f()
                if k > 0:
                    after(k - 1)
                if k == 2:
                    for d, h in FIRST:
                        sent.extend(rows_w.come(d, h, 0))
                if k == 9:
                    for d, h in SECOND:
                        sent.extend(rows_w.come(d, h, 0))

        ia, ib = 3 - i // 4, 3 - i % 4
        a, b = order(ia), order(ib)
        block = unit_kv(a, b)
        dp = dot(block, dT[...])
        u = ib * 4 + ia
        scale = jnp.exp(m_unit[u] - m_end) * inv
        p = E[pl.ds(pl.multiple_of(u * U, U), U), :].astype(F32) * scale
        g = (p * (dp - delta)).astype(BF)
        both = dot(g, qP[...]) + dot(p.astype(BF), dP[...])
        both = both.astype(BF)
        dkv[0, a, b] = both[0:512, :]
        dkv[1, a, b] = both[512:1024, :]
        kt = block.astype(F32).T.astype(BF)[0:64, :]
        dqT[...] += dot(kt, g)
        return 0

    ar_1()
    lax.fori_loop(0, 16, bwd, 0)

    grad = dqT[...]
    grad = jnp.concatenate([grad[:, 0:T], grad[:, T:]], axis=0).T.astype(BF)
    dqs[...] = grad
    for j in (4, 3, 5, 2, 6, 1, 7):
        to = (at.tp + j) % 8
        sent.append(net.push(
            dqs.at[pl.ds(pl.multiple_of(to * 64, 64), 64), :],
            dq_loc.at[at.tp], r_dq.at[8 - j], tp=to,
        ))
    dq_loc[at.tp] = dqs[pl.ds(pl.multiple_of(at.tp * 64, 64), 64), :]
    after(15)
    for j in (4, 3, 5, 2, 6, 1, 7):
        to = (at.tp + j) % 8
        sent.append(net.push(
            fin.at[pl.ds(pl.multiple_of(to * 128, 128), 128), :],
            back.at[at.tp], r_dkv.at[8 - j], tp=to,
        ))
    back[at.tp] = fin[pl.ds(pl.multiple_of(at.tp * 128, 128), 128), :]
    ar_5()
    for d, h in SIBS:
        rows_w.come(d, h, 1)
    for j in range(1, 8):
        frm = (at.tp + j) % 8
        net.arrive(dq_loc.at[frm], r_dq.at[j])
    for j in range(1, 8):
        frm = (at.tp + j) % 8
        net.arrive(back.at[frm], r_dkv.at[j])
    for g in range(4):
        even, odd = back[2 * g].astype(F32), back[2 * g + 1].astype(F32)
        dkv_loc[:, 128 * g : 128 * g + 128] = jnp.where(low, even, pltpu.roll(odd, 64, 1)).astype(BF)
        dkv_loc[:, 512 + 128 * g : 640 + 128 * g] = jnp.where(low, pltpu.roll(even, 64, 1), odd).astype(BF)
    net.sent(sent)


def mega(target, source, gain_t, gain_s, wq, wk, wv, wo, go):
    any_ = pl.BlockSpec(memory_space=pl.ANY)
    vmem = pl.BlockSpec(memory_space=pltpu.VMEM)
    V, D, S = pltpu.VMEM, pltpu.SemaphoreType.DMA, jax.ShapeDtypeStruct
    return pl.pallas_call(
        kernel,
        out_shape=(S((8, 4096, 128), BF), S((128, 4096), BF), S((8, 64, 128), BF), S((128, 1024), BF)),
        in_specs=[any_] * 9,
        out_specs=[any_, vmem, vmem, vmem],
        scratch_shapes=[
            V((16384, TT), BF),
            V((16384, 128), BF),
            V((2048, 1024), BF),
            V((2, 4, 4, 512, 128), BF),
            V((2, 2, 4, 256, 128), BF),
            V((2, 2, 4, 512, 128), BF),
            V((2, 2, 256, 128), BF),
            V((2, 2, 512, 128), BF),
            V((2, 4, 128, 512), BF),
            V((2, 4, 128, 128), BF),
            V((128, TT), BF), V((TT, 128), BF), V((128, TT), BF), V((TT, 128), BF),
            V((80, TT), F32), V((1, TT), F32), V((16, 1, TT), F32), V((64, TT), F32),
            V((128, T), BF),
            V((8, 128, 128), BF), V((8, 128, 128), BF), V((1024, 128), BF), V((T, 128), BF),
            V((64, 4096), BF), V((128, 4096), BF),
            V((1, 4096), F32), V((1, 4096), F32),
            D((256,)), D((32,)), D((4, 2, 2)), D((4, 2, 2)), D((4, 2, 2)), D((8,)), D((2, 4, 4, 2)),
            D((2, 2, 4)), D((2, 2, 4)), D((2, 2)), D((2, 2)), D((4, 2, 4)), D((8,)), D((8,)),
        ],
        compiler_params=pltpu.CompilerParams(
            collective_id=0, has_side_effects=True, vmem_limit_bytes=67043328
        ),
    )(target, source, gain_t.reshape(1, -1), gain_s.reshape(1, -1), wq, wk, wv, wo, go)


def norm_back(matrix, scaling, upstream):
    widened = matrix.astype(F32)
    factor = lax.rsqrt(jnp.mean(widened * widened, axis=-1, keepdims=True) + EPS)
    weighted = upstream * scaling
    inner = jnp.mean(widened * weighted, axis=-1, keepdims=True)
    return factor * weighted - widened * factor * factor * factor * inner


def shards(target, source, gain_t, gain_s, wq, wk, wv, wo, go):
    wq_all, gop, dq, dkv = mega(target, source, gain_t, gain_s, wq, wk, wv, wo, go)
    grad_xn = lax.dot_general(dq, wq_all, (((0, 2), (0, 2)), ((), ())), preferred_element_type=F32)
    grad_target = norm_back(target, gain_t, grad_xn)
    grad_sn = dot_t(dkv[:, :512], wk) + dot_t(dkv[:, 512:], wv)
    grad_source = norm_back(source, gain_s, grad_sn)
    return grad_target, grad_source, gop.astype(F32)


def solution(mesh):
    rows = P(("sp", "tp"), None)
    return jax.shard_map(
        shards,
        mesh=mesh,
        in_specs=(rows, rows, P(), P(), P(None, "tp"), P(), P(), P("tp", None), rows),
        out_specs=(rows, rows, P("tp", None)),
        check_vma=False,
    )
```

```python
import functools

import jax
import jax.numpy as jnp
from jax import lax
from jax.experimental import pallas as pl
from jax.experimental.pallas import tpu as pltpu
from jax.sharding import PartitionSpec as P

BF = jnp.bfloat16
F32 = jnp.float32
EPS = 1e-06
MESH = pl.DeviceIdType.MESH

T = 512
TT = 2 * T
U = 1024
TG0 = 6144
XN0 = 4096


def dot(a, b):
    return jnp.dot(a, b, preferred_element_type=F32)


def dot_t(a, b):
    return lax.dot_general(a, b, (((1,), (1,)), ((), ())), preferred_element_type=F32)


def normalize(rows, gain):
    wide = rows.astype(F32)
    factor = lax.rsqrt(jnp.mean(wide * wide, axis=-1, keepdims=True) + EPS)
    return (wide * factor * gain).astype(BF)


def order(i):
    return i + i // 2 - 2 * (i // 3)


class Coords:
    def __init__(self):
        self.sp = lax.axis_index("sp")
        self.tp = lax.axis_index("tp")
        self.z, self.x = self.sp // 4, self.sp % 4
        self.y, self.c = self.tp // 2, self.tp % 2

    def block(self, half, a, b):
        if half == 0:
            return ((self.z + b) % 4) * 4 + (self.x + a) % 4
        return ((self.z + a) % 4) * 4 + (self.x + b) % 4

    def ring(self, d, sib):
        return ((self.y + d) % 4) * 2 + (self.c if sib == 0 else 1 - self.c)


class Net:
    def __init__(self, at, send_sems, stand_in):
        self.at, self.sems, self.count, self.stand_in = at, send_sems, 0, stand_in

    def push(self, src, dst, recv, sp=None, tp=None):
        number = self.count
        sem = self.sems.at[number]
        self.count += 1
        who = (self.at.sp if sp is None else sp, self.at.tp if tp is None else tp)
        copy = pltpu.make_async_remote_copy(
            src_ref=src, dst_ref=dst, send_sem=sem, recv_sem=recv, device_id=who, device_id_type=MESH
        )
        copy.start()
        return number, src.shape

    def sent(self, copies):
        for number, (rows, columns) in copies:
            place = self.stand_in.at[pl.ds(0, rows), pl.ds(0, columns)]
            pltpu.make_async_remote_copy(
                src_ref=place, dst_ref=place, send_sem=self.sems.at[number], recv_sem=self.sems.at[number],
                device_id=(self.at.sp, self.at.ring(1, 0)), device_id_type=MESH,
            ).wait_send()

    def arrive(self, dst, recv):
        pltpu.make_async_remote_copy(
            src_ref=dst, dst_ref=dst, send_sem=self.sems.at[0], recv_sem=recv,
            device_id=(self.at.sp, self.at.ring(1, 0)), device_id_type=MESH,
        ).wait_recv()


class RowsGather:
    def __init__(self, net, place, recv):
        self.net, self.place, self.recv = net, place, recv

    def send(self, d, h, way):
        at = self.net.at
        src = self.place(at.ring(d, 0), h)
        if way == 0:
            return self.net.push(src, src, self.recv.at[d, 1, h], tp=at.ring(0, 1))
        return self.net.push(src, src, self.recv.at[(d - way) % 4, 0, h], tp=at.ring(way, 0))

    def begin_first(self):
        return [self.send(0, 0, 1), self.send(0, 1, -1)]

    def begin_rest(self):
        s = self.send
        return [s(0, 1, 1), s(0, 0, -1), s(0, 0, 0), s(0, 1, 0)]

    def begin(self):
        return self.begin_first() + self.begin_rest()

    def come(self, d, h, sib):
        at = self.net.at
        self.net.arrive(self.place(at.ring(d, sib), h), self.recv.at[d, sib, h])
        sent = []
        if sib == 0:
            if (d, h) == (3, 0):
                sent.append(self.send(d, h, 1))
            if (d, h) == (1, 1):
                sent.append(self.send(d, h, -1))
            sent.append(self.send(d, h, 0))
        return sent


FIRST = [(3, 0), (1, 1)]
SECOND = [(3, 1), (1, 0), (2, 0), (2, 1)]
SIBS = [(0, 0), (0, 1), (3, 0), (1, 1), (3, 1), (1, 0), (2, 0), (2, 1)]


class PairsGather:
    def __init__(self, net, kv, recv):
        self.net, self.kv, self.recv = net, kv, recv

    def rows(self, half, a, b, piece):
        start = self.net.at.block(half, a, b) * 1024 + half * 512 + piece * 256
        return self.kv.at[pl.ds(pl.multiple_of(start, 256), 256), :]

    def send(self, half, a, b, piece, axis, way):
        at = self.net.at
        src = self.rows(half, a, b, piece)
        if axis == 0:
            to, a2, b2 = at.block(half, way, 0), (a - way) % 4, b
        else:
            to, a2, b2 = at.block(half, 0, way), a, (b - way) % 4
        return self.net.push(src, src, self.recv.at[half, a2, b2, piece], sp=to)

    def begin(self):
        sent = []
        for piece, way in ((0, 1), (1, -1), (1, 1), (0, -1)):
            for half in (0, 1):
                sent.append(self.send(half, 0, 0, piece, 0, way))
        return sent

    def begin_second(self):
        sent = []
        for piece, way in ((0, 1), (1, -1), (1, 1), (0, -1)):
            for half in (0, 1):
                sent.append(self.send(half, 0, 0, piece, 1, way))
        return sent

    def come(self, a, b, piece):
        sent = []
        for half in (0, 1):
            self.net.arrive(self.rows(half, a, b, piece), self.recv.at[half, a, b, piece])
            if b == 0:
                if (a, piece) == (3, 0):
                    sent.append(self.send(half, a, b, piece, 0, 1))
                if (a, piece) == (1, 1):
                    sent.append(self.send(half, a, b, piece, 0, -1))
                for way in (1, -1):
                    sent.append(self.send(half, a, b, piece, 1, way))
            else:
                if (b, piece) == (3, 0):
                    sent.append(self.send(half, a, b, piece, 1, 1))
                if (b, piece) == (1, 1):
                    sent.append(self.send(half, a, b, piece, 1, -1))
        return sent


PHASE1 = [(3, 0, 0), (1, 0, 1), (3, 0, 1), (1, 0, 0), (2, 0, 0), (2, 0, 1)]
PHASE2 = (
    [(0, 3, 0), (0, 1, 1), (0, 3, 1), (0, 1, 0)]
    + [e for a in (3, 1) for e in ((a, 3, 0), (a, 1, 1), (a, 3, 1), (a, 1, 0))]
    + [(0, 2, 0), (0, 2, 1)]
    + [(2, 3, 0), (2, 1, 1), (2, 3, 1), (2, 1, 0)]
    + [e for a in (3, 1, 2) for e in ((a, 2, 0), (a, 2, 1))]
)


def kernel(
    tgt, src, gain_t, gain_s, wq, wk, wv, wo, go,
    wq_all, gop, grad_t, grad_s,
    E, kv, gg, dkv, hop, end1, hop2, end2, ar1, ar2,
    qT, qP, dT, dP, acc, m_run, m_unit, s0, s1, top0, top1, oT, back, dq_loc,
    wo_v, gt_v, gs_v,
    send_sems, load_sems, r_xn, r_gg, r_wq, r_a2a, r_kv, r_rs1, r_rs2, r_rs3, r_rs4, r_ar, r_dq, r_dkv,
):
    src_v = gop
    arP = wo_v
    dqT = acc.at[pl.ds(0, 64), :]
    fin, dqs = qP, dP
    at = Coords()
    net = Net(at, send_sems, E)
    lane = lax.broadcasted_iota(jnp.int32, (1, 128), 1)
    low = lane < 64

    barrier = pltpu.get_barrier_semaphore()
    others = [(at.sp, (at.tp + j) % 8) for j in range(1, 8)]
    others += [(at.block(0, a, 0), at.tp) for a in (1, 2, 3)]
    others += [(at.block(0, 0, b), at.tp) for b in (1, 2, 3)]
    for who in others:
        pl.semaphore_signal(barrier, inc=1, device_id=who, device_id_type=MESH)

    gg_own = [
        pltpu.make_async_copy(
            go.at[:, pl.ds(1024 * k, 1024)],
            gg.at[pl.ds(pl.multiple_of(at.tp * 256 + 64 * k, 64), 64), :],
            load_sems.at[8 + k],
        )
        for k in range(4)
    ]
    loads = [
        pltpu.make_async_copy(gain_t, gt_v, load_sems.at[1]),
        pltpu.make_async_copy(src, src_v, load_sems.at[2]),
        pltpu.make_async_copy(gain_s, gs_v, load_sems.at[3]),
        pltpu.make_async_copy(wk, E.at[pl.ds(0, 4096), pl.ds(0, 512)], load_sems.at[4]),
        pltpu.make_async_copy(wv, E.at[pl.ds(0, 4096), pl.ds(512, 512)], load_sems.at[5]),
        pltpu.make_async_copy(wo, wo_v, load_sems.at[6]),
    ]
    loads_t = [
        pltpu.make_async_copy(
            tgt.at[:, pl.ds(1024 * k, 1024)], E.at[pl.ds(TG0 + 64 * k, 64), :], load_sems.at[12 + k]
        )
        for k in range(4)
    ]
    loads_w = [
        pltpu.make_async_copy(
            wq.at[pl.ds(512 * k, 512), :], dkv.at[0, k // 4, k % 4], load_sems.at[16 + k]
        )
        for k in range(8)
    ]
    for load in loads_t + loads + loads_w + gg_own:
        load.start()

    def xn_place(j, h):
        return E.at[pl.ds(pl.multiple_of(XN0 + j * 256 + h * 128, 128), 128), :]

    def gg_place(j, h):
        return gg.at[pl.ds(pl.multiple_of(j * 256 + h * 128, 128), 128), :]

    def wq_place(j, h):
        return wq_all.at[j, pl.ds(h * 2048, 2048), :]

    rows_x = RowsGather(net, xn_place, r_xn)
    rows_g = RowsGather(net, gg_place, r_gg)
    rows_w = RowsGather(net, wq_place, r_wq)

    for load in loads_t:
        load.wait()
    loads[0].wait()
    xn = normalize(jnp.concatenate([E[TG0 + 64 * k : TG0 + 64 * k + 64, :] for k in range(4)], axis=1), gt_v[...])
    for k in range(4):
        E[pl.ds(pl.multiple_of(XN0 + at.tp * 256 + 64 * k, 64), 64), :] = xn[:, 1024 * k : 1024 * k + 1024]
    pl.semaphore_wait(barrier, len(others))
    sent_x = rows_x.begin_first()

    loads[1].wait()
    loads[2].wait()
    sn = normalize(src_v[...], gs_v[...])
    loads[3].wait()
    loads[4].wait()
    pairs = dot(sn, E[0:4096, :])
    for g in range(4):
        kb = pairs[:, 128 * g : 128 * g + 128]
        vb = pairs[:, 512 + 128 * g : 512 + 128 * g + 128]
        dP[256 * g : 256 * g + 128, :] = jnp.where(low, kb, pltpu.roll(vb, 64, 1)).astype(BF)
        dP[256 * g + 128 : 256 * g + 256, :] = jnp.where(low, pltpu.roll(kb, 64, 1), vb).astype(BF)
    mine = kv.at[pl.ds(pl.multiple_of(at.sp * 1024 + at.tp * 128, 128), 128), :]
    sent, sent_a2a = [], []
    for j in (4, 3, 5, 2, 6, 1, 7):
        to = (at.tp + j) % 8
        place = dP.at[pl.ds(pl.multiple_of(to * 128, 128), 128), :]
        sent_a2a.append(net.push(place, mine, r_a2a.at[8 - j], tp=to))
    mine[...] = dP[pl.ds(pl.multiple_of(at.tp * 128, 128), 128), :]
    for d, h in FIRST:
        sent_x += rows_x.come(d, h, 0)
    sent_x += rows_x.begin_rest()
    for j in range(1, 8):
        frm = (at.tp + j) % 8
        net.arrive(kv.at[pl.ds(pl.multiple_of(at.sp * 1024 + frm * 128, 128), 128), :], r_a2a.at[j])
    pairs_g = PairsGather(net, kv, r_kv)
    sent += pairs_g.begin()
    for load in gg_own:
        load.wait()
    loads[5].wait()
    for load in loads_w:
        load.wait()
    own_w = [
        pltpu.make_async_copy(
            dkv.at[0, k // 4, k % 4], wq_all.at[at.tp, pl.ds(512 * k, 512), :], load_sems.at[24 + k]
        )
        for k in range(8)
    ]
    for copy in own_w:
        copy.start()

    for e in PHASE1[:2]:
        sent += pairs_g.come(*e)
    sent += pairs_g.begin_second()
    for e in PHASE1[2:4]:
        sent += pairs_g.come(*e)
    for d, h in SECOND[:2]:
        sent_x += rows_x.come(d, h, 0)
    for e in PHASE1[4:] + PHASE2[:2]:
        sent += pairs_g.come(*e)
    for d, h in SECOND[2:]:
        sent_x += rows_x.come(d, h, 0)
    for e in PHASE2[2:4]:
        sent += pairs_g.come(*e)
    for d, h in SIBS:
        rows_x.come(d, h, 1)

    def gathered(ref, base, k):
        return jnp.concatenate(
            [ref[base + j * 256 + k * 64 : base + j * 256 + k * 64 + 64, :] for j in range(8)], axis=0
        )

    def wq_rows(k):
        return jnp.concatenate([dkv[0, k // 2, 2 * (k % 2)], dkv[0, k // 2, 2 * (k % 2) + 1]], axis=0)

    q = dot(gathered(E, XN0, 0), wq_rows(0))
    for k in range(1, 4):
        q += dot(gathered(E, XN0, k), wq_rows(k))
    q = q.astype(BF).astype(F32)
    net.sent(sent_x + sent_a2a)

    for h, a in enumerate((jnp.where(low, q, 0.0), jnp.where(low, pltpu.roll(q, 64, 1), 0.0))):
        r = slice(h * T, h * T + T)
        qP[r, :] = a.astype(BF)
        qT[:, r] = (a * 0.125).T.astype(BF)

    acc[...] = jnp.zeros_like(acc)
    m_run[...] = jnp.full_like(m_run, -jnp.inf)
    ones = jnp.ones((16, 512), BF)
    work, tops = (s0, s1), (top0, top1)

    def kv_rows(half, a, b):
        start = pl.multiple_of(at.block(half, a, b) * 1024 + half * 512, 512)
        return kv[pl.ds(start, 512), :]

    def weights_at(half, u):
        return pl.ds(pl.multiple_of(u * U + half * 512, 512), 512)

    def scores(half, u):
        s = dot(kv_rows(half, order(u % 4), order(u // 4)), qT[...])
        work[half][...] = s
        tops[half][...] = jnp.max(s, axis=0, keepdims=True)

    def absorb(half, u):
        m_old = m_run[...]
        m_new = jnp.maximum(m_old, tops[half][...])
        shrink = jnp.exp(m_old - m_new)
        e = jnp.exp(work[half][...] - m_new).astype(BF)
        E[weights_at(half, u), :] = e
        m_run[...] = m_new
        m_unit[pl.ds(2 * u + half, 1)] = m_new[None]
        block = kv_rows(half, order(u % 4), order(u // 4))
        vt = block.astype(F32).T.astype(BF)[64:128, :]
        acc[...] = acc[...] * shrink + dot(jnp.concatenate([vt, ones], axis=0), e)

    def begin_w():
        for copy in own_w:
            copy.wait()
        sent.extend(rows_w.begin())

    def gg_come(places):
        for d, h in places:
            sent.extend(rows_g.come(d, h, 0))

    def pairs_come(places):
        for e in places:
            sent.extend(pairs_g.come(*e))

    heads = {
        0: lambda: (sent.extend(rows_g.begin()), pairs_come(PHASE2[4:8])),
        1: lambda: pairs_come(PHASE2[8:12]),
        2: lambda: pairs_come(PHASE2[12:15]),
        3: lambda: pairs_come(PHASE2[15:18]),
        5: lambda: pairs_come(PHASE2[18:20]),
        6: lambda: (gg_come(FIRST), pairs_come(PHASE2[20:22])),
        8: lambda: pairs_come(PHASE2[22:24]),
        10: lambda: gg_come(SECOND[:2]),
        14: lambda: (gg_come(SECOND[2:]), begin_w()),
    }

    def fwd(u, _):
        for k, f in heads.items():
            pl.when(u == k)(lambda f=f: f() and None)
        scores(1, u)
        absorb(0, u)
        scores(0, (u + 1) % 16)
        absorb(1, u)
        return 0

    scores(0, 0)
    lax.fori_loop(0, 16, fwd, 0)
    for d, h in SIBS:
        rows_g.come(d, h, 1)
    do = dot_t(gathered(gg, 0, 0), wo_v[:, 0:1024])
    for k in range(1, 4):
        do += dot_t(gathered(gg, 0, k), wo_v[:, 1024 * k : 1024 * k + 1024])
    do = do.astype(BF).astype(F32)

    for h, b in enumerate((jnp.where(low, 0.0, pltpu.roll(do, 64, 1)), jnp.where(low, 0.0, do))):
        r = slice(h * T, h * T + T)
        dP[r, :] = b.astype(BF)
        dT[:, r] = (b * 0.125).T.astype(BF)

    inv = 1.0 / acc[64:65, :]
    o = (acc[0:64, :] * inv).astype(BF)
    oT[0:64, :] = o[:, 0:T]
    oT[64:128, :] = o[:, T:]
    delta = jnp.sum(dT[64:128, :].astype(F32) * o.astype(F32), axis=0, keepdims=True)
    m_end = m_run[...]
    dqT[...] = jnp.zeros((64, TT), F32)

    for k in range(4):
        arP[:, 1024 * k : 1024 * k + 1024] = dot(oT[...], gathered(gg, 0, k)).astype(BF)

    def wide_col(half, a):
        pi = at.x if half == 0 else at.z
        return pl.ds(pl.multiple_of(half * 2048 + ((pi + a) % 4) * 512, 512), 512)

    def slim_col(half, b):
        pi, qi = (at.x, at.z) if half == 0 else (at.z, at.x)
        return pl.ds(pl.multiple_of(half * 2048 + pi * 512 + ((qi + b) % 4) * 128, 128), 128)

    def ar_1():
        for half in (0, 1):
            for a in (1, 3, 2):
                sent.append(net.push(arP.at[:, wide_col(half, a)], ar1.at[half, 3 - a], r_ar.at[0, half, 4 - a], sp=at.block(half, a, 0)))

    def ar_2():
        for half in (0, 1):
            total = arP[:, wide_col(half, 0)].astype(F32)
            for a in (1, 2, 3):
                net.arrive(ar1.at[half, a - 1], r_ar.at[0, half, a])
                total += ar1[half, a - 1].astype(F32)
            arP[:, wide_col(half, 0)] = total.astype(BF)
            for b in (1, 3, 2):
                sent.append(net.push(arP.at[:, slim_col(half, b)], ar2.at[half, 3 - b], r_ar.at[1, half, 4 - b], sp=at.block(half, 0, b)))

    def ar_3():
        for half in (0, 1):
            total = arP[:, slim_col(half, 0)].astype(F32)
            for b in (1, 2, 3):
                net.arrive(ar2.at[half, b - 1], r_ar.at[1, half, b])
                total += ar2[half, b - 1].astype(F32)
            gop[:, slim_col(half, 0)] = total.astype(BF)
            for b in (1, 3, 2):
                place = gop.at[:, slim_col(half, 0)]
                sent.append(net.push(place, place, r_ar.at[2, half, 4 - b], sp=at.block(half, 0, b)))

    def ar_4():
        for half in (0, 1):
            for b in (1, 2, 3):
                net.arrive(gop.at[:, slim_col(half, b)], r_ar.at[2, half, b])
            for a in (1, 3, 2):
                place = gop.at[:, wide_col(half, 0)]
                sent.append(net.push(place, place, r_ar.at[3, half, 4 - a], sp=at.block(half, a, 0)))

    def ar_5():
        for half in (0, 1):
            for a in (1, 2, 3):
                net.arrive(gop.at[:, wide_col(half, a)], r_ar.at[3, half, a])

    def add_to(place, arrived):
        place[...] = (place[...].astype(F32) + arrived[...].astype(F32)).astype(BF)

    def back_place(i):
        group = i // 4
        mid = (group + 1) // 2 % 2
        ia = mid * (2 - i % 2) + (1 - mid) * (3 - group)
        ib = mid * (3 - (i + 4) // 2 + 4) + (1 - mid) * (3 - i % 4)
        return order(ia), order(ib), ib * 4 + ia

    def after(i):
        a, b, _ = back_place(i)
        for half in (0, 1):
            piece = dkv.at[half, a, b]
            top, bottom = piece.at[pl.ds(0, 256), :], piece.at[pl.ds(256, 256), :]
            plus, minus = at.block(half, 1, 0), at.block(half, 3, 0)
            plus2, minus2 = at.block(half, 0, 1), at.block(half, 0, 3)
            if a == 2:
                sent.append(net.push(top, hop.at[half, 0, b], r_rs1.at[half, 0, b], sp=plus))
                sent.append(net.push(bottom, hop.at[half, 1, b], r_rs1.at[half, 1, b], sp=minus))
            elif a == 3:
                net.arrive(hop.at[half, 1, b], r_rs1.at[half, 1, b])
                add_to(bottom, hop.at[half, 1, b])
                sent.append(net.push(piece, end1.at[half, 1, b], r_rs2.at[half, 1, b], sp=minus))
            elif a == 1:
                net.arrive(hop.at[half, 0, b], r_rs1.at[half, 0, b])
                add_to(top, hop.at[half, 0, b])
                sent.append(net.push(piece, end1.at[half, 0, b], r_rs2.at[half, 0, b], sp=plus))
            else:
                total = piece[...].astype(F32)
                for side in (0, 1):
                    net.arrive(end1.at[half, side, b], r_rs2.at[half, side, b])
                    total += end1[half, side, b].astype(F32)
                if b == 2:
                    piece[...] = total.astype(BF)
                    sent.append(net.push(top, hop2.at[half, 0], r_rs3.at[half, 0], sp=plus2))
                    sent.append(net.push(bottom, hop2.at[half, 1], r_rs3.at[half, 1], sp=minus2))
                elif b == 3:
                    piece[...] = total.astype(BF)
                    net.arrive(hop2.at[half, 1], r_rs3.at[half, 1])
                    add_to(bottom, hop2.at[half, 1])
                    sent.append(net.push(piece, end2.at[half, 1], r_rs4.at[half, 1], sp=minus2))
                elif b == 1:
                    piece[...] = total.astype(BF)
                    net.arrive(hop2.at[half, 0], r_rs3.at[half, 0])
                    add_to(top, hop2.at[half, 0])
                    sent.append(net.push(piece, end2.at[half, 0], r_rs4.at[half, 0], sp=plus2))
                else:
                    for side in (0, 1):
                        net.arrive(end2.at[half, side], r_rs4.at[half, side])
                        total += end2[half, side].astype(F32)
                    fin[half * 512 : half * 512 + 512, :] = total.astype(BF)

    def projected(half, i):
        a, b, _ = back_place(i)
        work[half][...] = dot(kv_rows(half, a, b), dT[...])

    def gradients(half, i):
        a, b, u = back_place(i)
        scale = jnp.exp(m_unit[2 * u + half] - m_end) * inv
        p = E[weights_at(half, u), :].astype(F32) * scale
        g = (p * (work[half][...] - delta)).astype(BF)
        dkv[half, a, b] = (dot(g, qP[...]) + dot(p.astype(BF), dP[...])).astype(BF)
        kt = kv_rows(half, a, b).astype(F32).T.astype(BF)[0:64, :]
        dqT[...] += dot(kt, g)

    def spare(i, c):
        return back_place(i)[2] * U + c

    def loads_last(k):
        if 2 <= k < 6:
            c = k - 2
            return [
                pltpu.make_async_copy(
                    w.at[pl.ds(1024 * c, 1024), :],
                    E.at[pl.ds(spare(c, 0), 1024), pl.ds(512 * n, 512)],
                    load_sems.at[8 * n + c],
                )
                for n, w in enumerate((wk, wv))
            ]
        if k == 6:
            return [
                pltpu.make_async_copy(
                    rows.at[:, pl.ds(1024 * c, 1024)],
                    E.at[pl.ds(spare(4, first + count * c), count), :],
                    load_sems.at[16 + c + n],
                )
                for rows, first, count, n in ((src, 0, 128, 0), (tgt, 512, 64, 4))
                for c in range(4)
            ]
        if k in (14, 15):
            return [
                pltpu.make_async_copy(
                    wq_all.at[j, pl.ds(1024 * c, 1024), :],
                    E.at[pl.ds(spare(5 + c, 0), 1024), pl.ds(128 * j, 128)],
                    load_sems.at[32 + 8 * c + j],
                )
                for c in ((0, 1) if k == 14 else (2, 3))
                for j in range(8)
            ]
        return []

    def load_ahead(k):
        for copy in loads_last(k):
            copy.start()

    def bwd(i, _):
        for k in range(16):
            if k == 3:
                extra = [ar_2]
            elif k == 6:
                extra = [ar_3]
            elif k == 8:
                extra = [ar_4]
            else:
                extra = []

            @pl.when(i == k)
            def _(k=k, extra=extra):
                load_ahead(k)
                for f in extra:
                    f()
                if k > 0:
                    after(k - 1)
                if k == 3:
                    for d, h in FIRST:
                        sent.extend(rows_w.come(d, h, 0))
                if k == 6:
                    for d, h in SECOND[:2]:
                        sent.extend(rows_w.come(d, h, 0))
                if k == 11:
                    for d, h in SECOND[2:]:
                        sent.extend(rows_w.come(d, h, 0))
                if k == 13:
                    for d, h in SIBS:
                        rows_w.come(d, h, 1)

        projected(1, i)
        gradients(0, i)
        projected(0, (i + 1) % 16)
        gradients(1, i)
        return 0

    ar_1()
    projected(0, 0)
    lax.fori_loop(0, 16, bwd, 0)

    grad = dqT[...]
    grad = jnp.concatenate([grad[:, 0:T], grad[:, T:]], axis=0).T.astype(BF)
    dqs[0:T, :] = grad
    for j in (4, 3, 5, 2, 6, 1, 7):
        to = (at.tp + j) % 8
        sent.append(net.push(
            dqs.at[pl.ds(pl.multiple_of(to * 64, 64), 64), :],
            dq_loc.at[at.tp], r_dq.at[8 - j], tp=to,
        ))
    dq_loc[at.tp] = dqs[pl.ds(pl.multiple_of(at.tp * 64, 64), 64), :]
    after(15)
    for j in (4, 3, 5, 2, 6, 1, 7):
        to = (at.tp + j) % 8
        sent.append(net.push(
            fin.at[pl.ds(pl.multiple_of(to * 128, 128), 128), :],
            back.at[at.tp], r_dkv.at[8 - j], tp=to,
        ))
    back[at.tp] = fin[pl.ds(pl.multiple_of(at.tp * 128, 128), 128), :]
    for j in range(1, 8):
        frm = (at.tp + j) % 8
        net.arrive(dq_loc.at[frm], r_dq.at[j])
    for k in range(16):
        for copy in loads_last(k):
            copy.wait()

    def finish(rows, x_of, gain, up_of, buf, out, sems):
        squares = jnp.zeros((rows, 1), F32)
        inner = jnp.zeros((rows, 1), F32)
        for c in range(4):
            x = x_of(c).astype(F32)
            weighted = up_of(c) * gain[:, 1024 * c : 1024 * c + 1024]
            buf[rows * c : rows * c + rows, :] = weighted
            squares += jnp.sum(x * x, axis=-1, keepdims=True)
            inner += jnp.sum(x * weighted, axis=-1, keepdims=True)
        factor = lax.rsqrt(squares / 4096 + EPS)
        pull = factor * factor * factor * (inner / 4096)
        copies = []
        for c in range(4):
            r = slice(rows * c, rows * c + rows)
            buf[r, :] = factor * buf[r, :] - x_of(c).astype(F32) * pull
            copies.append(pltpu.make_async_copy(
                buf.at[pl.ds(rows * c, rows), :], out.at[:, pl.ds(1024 * c, 1024)], load_sems.at[sems + c]
            ))
            copies[-1].start()
        return copies

    dq_rows = jnp.concatenate([dq_loc[j] for j in range(8)], axis=1)
    outs = finish(
        64, lambda c: E[pl.ds(spare(4, 512 + 64 * c), 64), :], gt_v,
        lambda c: dot_t(dq_rows, E[pl.ds(spare(5 + c, 0), 1024), :]), s1, grad_t, 64,
    )
    for j in range(1, 8):
        frm = (at.tp + j) % 8
        net.arrive(back.at[frm], r_dkv.at[j])
    keys, values = [], []
    for g in range(4):
        even, odd = back[2 * g].astype(F32), back[2 * g + 1].astype(F32)
        keys.append(jnp.where(low, even, pltpu.roll(odd, 64, 1)).astype(BF))
        values.append(jnp.where(low, pltpu.roll(even, 64, 1), odd).astype(BF))
    dkv_rows = jnp.concatenate(keys + values, axis=1)
    outs += finish(
        128, lambda c: E[pl.ds(spare(4, 128 * c), 128), :], gs_v,
        lambda c: dot_t(dkv_rows, E[pl.ds(spare(c, 0), 1024), :]), s0, grad_s, 68,
    )
    ar_5()
    for copy in outs:
        copy.wait()
    net.sent(sent)


def mega(target, source, gain_t, gain_s, wq, wk, wv, wo, go):
    any_ = pl.BlockSpec(memory_space=pl.ANY)
    vmem = pl.BlockSpec(memory_space=pltpu.VMEM)
    V, D, S = pltpu.VMEM, pltpu.SemaphoreType.DMA, jax.ShapeDtypeStruct
    return pl.pallas_call(
        kernel,
        out_shape=(S((8, 4096, 128), BF), S((128, 4096), BF), S((64, 4096), F32), S((128, 4096), F32)),
        in_specs=[any_] * 9,
        out_specs=[any_, vmem, any_, any_],
        scratch_shapes=[
            V((16384, TT), BF),
            V((16384, 128), BF),
            V((2048, 1024), BF),
            V((2, 4, 4, 512, 128), BF),
            V((2, 2, 4, 256, 128), BF),
            V((2, 2, 4, 512, 128), BF),
            V((2, 2, 256, 128), BF),
            V((2, 2, 512, 128), BF),
            V((2, 3, 128, 512), BF),
            V((2, 3, 128, 128), BF),
            V((128, TT), BF), V((TT, 128), BF), V((128, TT), BF), V((TT, 128), BF),
            V((80, TT), F32), V((1, TT), F32), V((32, 1, TT), F32),
            V((512, TT), F32), V((512, TT), F32), V((1, TT), F32), V((1, TT), F32),
            V((128, T), BF),
            V((8, 128, 128), BF), V((8, 64, 128), BF),
            V((128, 4096), BF),
            V((1, 4096), F32), V((1, 4096), F32),
            D((256,)), D((80,)), D((4, 2, 2)), D((4, 2, 2)), D((4, 2, 2)), D((8,)), D((2, 4, 4, 2)),
            D((2, 2, 4)), D((2, 2, 4)), D((2, 2)), D((2, 2)), D((4, 2, 4)), D((8,)), D((8,)),
        ],
        compiler_params=pltpu.CompilerParams(
            collective_id=0, has_side_effects=True, vmem_limit_bytes=67043328
        ),
    )(target, source, gain_t.reshape(1, -1), gain_s.reshape(1, -1), wq, wk, wv, wo, go)


def shards(*args):
    _, grad_out_proj, grad_target, grad_source = mega(*args)
    return grad_target, grad_source, grad_out_proj.astype(F32)


def solution(mesh):
    rows = P(("sp", "tp"), None)
    return jax.shard_map(
        shards,
        mesh=mesh,
        in_specs=(rows, rows, P(), P(), P(None, "tp"), P(), P(), P("tp", None), rows),
        out_specs=(rows, rows, P("tp", None)),
        check_vma=False,
    )
```
